512 devices in a mesh: sp: 32 (over z, core), tp: 16 (over y, x).
Axes of the slice: x: 4, y: 4, z: 16, core: 2. Of those that a mesh axis runs over, the one named last changes fastest.
Arguments:
- residual: bfloat16 [4096, 4096], P('sp', 'tp'), may hold values from -46 to 46
- query_small: bfloat16 [4096, 2048], P('sp', 'tp'), may hold values from -6 to 6
- key_narrow_group: bfloat16 [4096, 2048], P('sp', 'tp'), may hold values from -6 to 6
- query_large: bfloat16 [4096, 4096], P('sp', 'tp'), may hold values from -6 to 6
- key_large: bfloat16 [4096, 4096], P('sp', 'tp'), may hold values from -6 to 6
- values: bfloat16 [4096, 2, 2048], P('sp', None, 'tp'), may hold values from -6 to 6
- gates: bfloat16 [4096, 2, 2048], P('sp', None, 'tp'), may hold values from -6 to 6
- log_decay: float32 [4096, 2, 16], P('sp', None, 'tp'), may hold values from -0.65 to 0, as said below
- head_gain: float32 [2, 2048], P(None, 'tp'), may hold values from 0.1 to 1.9
- out_weight: bfloat16 [2, 2048, 4096], P(None, 'sp', 'tp'), may hold values from -0.09375 to 0.09375
- norm_gain: float32 [4096], P('tp'), may hold values from 0.1 to 1.9
- routes: int32 [4096, 2], P('sp'), may hold values from 0 to 31, all different within a row; in each aligned block of 128 rows (0 to 127, 128 to 255, ...) at most 16 rows name the same one
- route_weight: float32 [4096, 2], P('sp'), may hold values from 0.2 to 1
- expert_gate: bfloat16 [32, 4096, 2048], P('sp', None, 'tp'), may hold values from -0.09375 to 0.09375
- expert_up: bfloat16 [32, 4096, 2048], P('sp', None, 'tp'), may hold values from -0.09375 to 0.09375
- expert_down: bfloat16 [32, 2048, 4096], P('sp', None, 'tp'), may hold values from -0.5 to 0.5
Outputs:
- new_stream: bfloat16 [4096, 4096], P('sp', 'tp')
The draws below stay inside these ranges and needn't reach their ends.
Inputs may be any that keep to these rules, and one draw needn't show every extreme that they name: `routes`: each row names two different experts; in each aligned block of 128 rows no expert is named more than 16 times, a bound that some block reaches. `log_decay`: negative at every position.
All inputs are finite; a program needn't handle non-finite values.
Results may differ from the reference program's by a relative error of at most 0.019.
Values may be sent and summed in bfloat16 or wider, within the bound.
A program may use at most 64 MiB of HBM per device.

```python
import math
import jax
import jax.numpy as jnp
import numpy as np
from jax import lax

D = 4096
H = 16
DKA = 128
DKB = 256
DV = 128
FF = 2048
TOK_DEV = 128
TOKENS = 4096
EXPERTS = 32
CAP = 16
N_SP = 32


def draw_residual(key, part):
    keys = jax.random.split(key, 3)
    base = jnp.clip(jax.random.normal(keys[0], (TOKENS, D), jnp.float32), -5.0, 5.0)
    ramp = jnp.arange(D, dtype=jnp.float32) / D
    coarse_estimate = jax.random.uniform(keys[1], (1, D), jnp.float32, 0.5, 1.5)
    columns = 0.3 * jnp.power(10.0, ramp)
    row_scale = jnp.exp(jax.random.uniform(keys[2], (TOKENS, 1), jnp.float32, -0.7, 0.7))
    return (base * columns[None, :] * coarse_estimate * row_scale).astype(jnp.bfloat16)


def draw_log_decay(key, part):
    keys = jax.random.split(key, 7)
    choose = jax.random.uniform(keys[0], (1, 2, H), jnp.float32)
    slow_heads = choose < 0.5
    fast_rate = jnp.exp(-jax.random.uniform(keys[1], (1, 2, H), jnp.float32, 3.4, 4.1))
    slow_rate = jax.random.uniform(keys[2], (1, 2, H), jnp.float32, 0.1, 0.4) / TOKENS
    decay_speed = jnp.where(slow_heads, slow_rate, fast_rate)
    block_count = TOKENS // TOK_DEV
    multiplier_term = jnp.exp(jax.random.uniform(keys[3], (block_count, 1, 1), jnp.float32, -0.69, 0.69))
    multiplier_term = jnp.repeat(multiplier_term, TOK_DEV, axis=0)
    coarse_estimate = jax.random.uniform(keys[4], (TOKENS, 2, H), jnp.float32, 0.5, 1.5)
    spots = jax.random.randint(keys[5], (3,), 0, TOKENS)
    hit_marker = jnp.any(jnp.arange(TOKENS)[:, None] == spots[None, :], axis=1)
    kept_fraction = jax.random.uniform(keys[6], (TOKENS, 1, 1), jnp.float32, 0.6, 0.8)
    spike_amount = jnp.where(hit_marker[:, None, None], jnp.log(kept_fraction), 0.0)
    return (-decay_speed * multiplier_term * coarse_estimate + spike_amount).astype(jnp.float32)


def levels(stream_key, shape, cuts, smallest, high):
    def one(dim, parts):
        draws = jax.random.uniform(jax.random.fold_in(jax.random.fold_in(stream_key, 6), dim), (parts,), jnp.float32, smallest / len(cuts), high / len(cuts))
        return jnp.repeat(jnp.exp(draws), shape[dim] // parts).reshape((-1,) + (1,) * (len(shape) - dim - 1))

    level = one(*cuts[0])
    for cut in cuts[1:]:
        level = level * one(*cut)
    return level


def shared_out(rng, own, number, rows, count, top, reach, slope):
    order = jax.random.permutation(rng, count)
    packed, usual = portions_of(count, rows * top, reach, slope, True), portions_of(count, rows * top, reach, slope, False)
    places = jnp.arange(count)

    def named(lengths, rotation):
        used = int((lengths > 0).sum())
        fixed = max(1, used // 4)
        moved = fixed + (places - fixed + rotation * (used - fixed)) % max(1, count - fixed)
        return jnp.zeros((count,), jnp.int32).at[order[jnp.where(places < fixed, places, moved)]].set(jnp.asarray(lengths, jnp.int32))

    lengths = jnp.where(number % 4 == 0, named(packed, number // 4), named(usual, number - number // 4 - 1))
    mixed = jax.random.permutation(jax.random.fold_in(own, 3), count)
    donor, sink = mixed[0:count // 2 * 2:2], mixed[1:count // 2 * 2:2]
    margin = jnp.minimum(lengths[donor] - 1, reach - lengths[sink]) // 2
    margin = jnp.where((donor == order[0]) | (sink == order[0]) | (lengths[sink] == 0), 0, jnp.maximum(margin, 0))
    moved = jax.random.randint(jax.random.fold_in(own, 4), (count // 2,), 0, 1 << 20) % (margin + 1)
    lengths = lengths.at[donor].add(-moved).at[sink].add(moved)
    items = jnp.searchsorted(jnp.cumsum(lengths), jnp.arange(rows * top), side="right").astype(jnp.int32)
    listing = items.reshape(top, rows).T
    listing = listing[jax.random.permutation(jax.random.fold_in(own, 1), rows)]
    rotation = jax.random.randint(jax.random.fold_in(own, 2), (rows, 1), 0, top)
    return jnp.take_along_axis(listing, (jnp.arange(top)[None, :] + rotation) % top, axis=1)


def portions_of(amount, total, reach, skew, full):
    weights = [(1 << 20) // math.isqrt(grade ** skew) + 1 for grade in range(1, amount + 1)]
    largest = reach if full else min(reach, max(-(-total // amount), total * weights[0] // sum(weights)))
    least = 1 if total - largest >= amount - 1 else 0
    given, spare = [largest] + [least] * (amount - 1), total - largest - least * (amount - 1)
    while spare > 0:
        candidates = [i for i in range(1, amount) if given[i] < largest] or [i for i in range(1, amount) if given[i] < reach]
        whole, left = sum([weights[i] for i in candidates]), spare
        for i in candidates:
            extra = min(reach - given[i], max(1, left * weights[i] // whole), spare)
            given[i] = given[i] + extra
            spare = spare - extra
    return np.array(given)


def scatter_about(own_key, dims, scale, most, cuts=(), held_as=jnp.bfloat16):
    result = jax.random.normal(own_key, dims, jnp.float32) * scale
    if len(cuts) > 0:
        result = levels(own_key, dims, cuts, -0.22, 0.18) * result
    return jnp.clip(result, min=-most, max=most).astype(held_as)


def setup_inputs(seed: int = 0) -> dict:
    key_of = jax.random.split(jax.random.key(seed), 17)
    residual = draw_residual(jax.random.fold_in(key_of[16], 71), 0)
    query_small = scatter_about(key_of[1], (TOKENS, H * DKA), 1.0, 6.0, ((0, 32), (1, 16)))
    key_narrow_group = scatter_about(key_of[2], (TOKENS, H * DKA), 1.0, 6.0, ((0, 32), (1, 16)))
    query_large = scatter_about(key_of[3], (TOKENS, H * DKB), 1.0, 6.0, ((0, 32), (1, 16)))
    key_large = scatter_about(key_of[4], (TOKENS, H * DKB), 1.0, 6.0, ((0, 32), (1, 16)))
    values = scatter_about(key_of[5], (TOKENS, 2, H * DV), 1.0, 6.0, ((0, 32), (2, 16)))
    gates = scatter_about(key_of[6], (TOKENS, 2, H * DV), 1.0, 6.0, ((0, 32), (2, 16)))
    log_decay = draw_log_decay(jax.random.fold_in(key_of[16], 71), 0)
    head_gain = jnp.clip(1.0 + 0.18 * jax.random.normal(key_of[8], (2, H * DV), jnp.float32), 0.1, 1.9)
    out_weight = scatter_about(key_of[9], (2, H * DV, D), (2 * H * DV) ** -0.5, 0.09375, ((1, 32), (2, 16)))
    norm_gain = jnp.clip(1.0 + 0.18 * jax.random.normal(key_of[10], (D,), jnp.float32), 0.1, 1.9)
    routes_keys = jax.random.split(jax.random.fold_in(key_of[11], 1), TOKENS // TOK_DEV)
    routes_turns = jax.random.permutation(jax.random.fold_in(key_of[11], 3), TOKENS // TOK_DEV)
    routes = jax.vmap(lambda own, number: shared_out(jax.random.fold_in(key_of[11], 2), own, number, TOK_DEV, EXPERTS, 2, CAP, 2))(routes_keys, routes_turns).reshape((TOKENS, 2))
    route_weight = jnp.clip(0.2 + 0.8 * jax.random.uniform(key_of[12], (TOKENS, 2), jnp.float32) ** levels(key_of[12], (TOKENS, 2), ((0, 32),), -0.2, 0.2), 0.2, 1.0)
    expert_gate = scatter_about(key_of[13], (EXPERTS, D, FF), D ** -0.5, 0.09375, ((0, 32), (2, 16)))
    expert_up = scatter_about(key_of[14], (EXPERTS, D, FF), D ** -0.5, 0.09375, ((0, 32), (2, 16)))
    expert_down = scatter_about(key_of[15], (EXPERTS, FF, D), (FF // 16) ** -0.5, 0.5, ((0, 32), (2, 16)))
    return {"residual": residual, "query_small": query_small, "key_narrow_group": key_narrow_group, "query_large": query_large, "key_large": key_large, "values": values, "gates": gates, "log_decay": log_decay, "head_gain": head_gain, "out_weight": out_weight, "norm_gain": norm_gain, "routes": routes, "route_weight": route_weight, "expert_gate": expert_gate, "expert_up": expert_up, "expert_down": expert_down}


EPS = 1e-06
THETA = 10000.0

def rotate(block, positions):
    half_dim = block.shape[-1] // 2
    inverse = jnp.power(THETA, -jnp.arange(half_dim, dtype=jnp.float32) * 2.0 / block.shape[-1])
    angles = positions[:, None, None] * inverse
    cosine_val, sine_val = (jnp.cos(angles), jnp.sin(angles))
    lower_half, upper_half = (block[..., :half_dim], block[..., half_dim:])
    return jnp.concatenate([lower_half * cosine_val - upper_half * sine_val, upper_half * cosine_val + lower_half * sine_val], axis=-1)

def block_terms(rot_queries, rot_keys, value_heads, rates):
    count = rates.shape[0]
    decay_sum = jnp.cumsum(rates, axis=0)
    by_head = decay_sum.T
    causal = (jnp.arange(count)[:, None] >= jnp.arange(count)[None, :])[None]
    spread = by_head[:, :, None] - by_head[:, None, :]
    weight = jnp.where(causal, jnp.exp(jnp.where(causal, spread, 0.0)), 0.0)
    scores = jnp.einsum('ihd,jhd->hij', rot_queries.astype(jnp.float32), rot_keys.astype(jnp.float32))
    weighted = (scores * weight).astype(jnp.bfloat16)
    within = jnp.einsum('hij,jhv->ihv', weighted.astype(jnp.float32), value_heads.astype(jnp.float32))
    block_end = decay_sum[-1]
    carried = (rot_keys.astype(jnp.float32) * jnp.exp(block_end[None, :] - decay_sum)[:, :, None]).astype(jnp.bfloat16)
    update = jnp.einsum('jhd,jhv->hdv', carried.astype(jnp.float32), value_heads.astype(jnp.float32))
    return (within, decay_sum, jnp.exp(block_end), update)

def final_result(rot_queries, decay_sum, within, state_in, gate_part, gain_part):
    cross_part = jnp.einsum('ihd,hdv->ihv', rot_queries.astype(jnp.float32), state_in, precision=lax.Precision.HIGHEST) * jnp.exp(decay_sum)[:, :, None]
    retained = within + cross_part
    scaled = retained * lax.rsqrt(lax.optimization_barrier(jnp.mean(retained * retained, axis=-1, keepdims=True)) + EPS)
    count, head_count, value_size = retained.shape
    gated = jax.nn.silu(gate_part.astype(jnp.float32)).reshape(count, head_count, value_size)
    return (scaled * gain_part.reshape(head_count, value_size) * gated).reshape(count, -1).astype(jnp.bfloat16)

def group_out(queries, keys_in, value_part, gate_part, rates, gain_part, key_size):
    length = queries.shape[0]
    head_count = rates.shape[1]
    value_size = value_part.shape[1] // head_count
    positions = jnp.arange(length, dtype=jnp.float32)
    rot_queries = rotate(queries.astype(jnp.float32).reshape(length, head_count, key_size), positions).astype(jnp.bfloat16)
    rot_keys = (rotate(keys_in.astype(jnp.float32).reshape(length, head_count, key_size), positions) * key_size ** (-0.5)).astype(jnp.bfloat16)
    value_heads = value_part.reshape(length, head_count, value_size)
    block_count = length // TOK_DEV

    def split_blocks(array):
        return array.reshape((block_count, TOK_DEV) + array.shape[1:])

    def advance(state, inputs):
        block_q, block_k, block_v, block_rates, block_gate = inputs
        within, decay_sum, fall, update = block_terms(block_q, block_k, block_v, block_rates)
        output = final_result(block_q, decay_sum, within, state, block_gate, gain_part)
        return (fall[:, None, None] * state + update, output)
    start_state = jnp.zeros((head_count, key_size, value_size), jnp.float32)
    _, outputs = lax.scan(advance, start_state, (split_blocks(rot_queries), split_blocks(rot_keys), split_blocks(value_heads), split_blocks(rates), split_blocks(gate_part)))
    return outputs.reshape(length, head_count * value_size)

def reference(residual, query_small, key_narrow_group, query_large, key_large, values, gates, log_decay, head_gain, out_weight, norm_gain, routes, route_weight, expert_gate, expert_up, expert_down):
    out_small = group_out(query_small, key_narrow_group, values[:, 0], gates[:, 0], log_decay[:, 0], head_gain[0], DKA)
    out_large = group_out(query_large, key_large, values[:, 1], gates[:, 1], log_decay[:, 1], head_gain[1], DKB)
    mixed = (jnp.dot(out_small, out_weight[0], preferred_element_type=jnp.float32) + jnp.dot(out_large, out_weight[1], preferred_element_type=jnp.float32)).astype(jnp.bfloat16)
    stream = residual.astype(jnp.float32) + mixed.astype(jnp.float32)
    normed = (stream * lax.rsqrt(lax.optimization_barrier(jnp.mean(stream * stream, axis=-1, keepdims=True)) + EPS) * norm_gain[None, :]).astype(jnp.bfloat16)
    experts = N_SP
    capacity = 4 * TOK_DEV // experts
    one_hot = (routes[:, :, None] == jnp.arange(experts, dtype=jnp.int32)[None, None, :]).astype(jnp.int32)
    one_hot = one_hot.reshape(N_SP, 2 * TOK_DEV, experts)
    before = jnp.cumsum(one_hot, axis=1) - one_hot
    slot_index = lax.optimization_barrier(jnp.sum(before * one_hot, axis=2)).reshape(TOKENS, 2)
    block_index = (jnp.arange(TOKENS, dtype=jnp.int32) // TOK_DEV).astype(jnp.int32)
    row_slot = (block_index[:, None] * capacity + slot_index).astype(jnp.int32)
    buffer = jnp.zeros((experts, N_SP * capacity, D), jnp.bfloat16)
    buffer = buffer.at[routes, row_slot].set(jnp.broadcast_to(normed[:, None, :], (TOKENS, 2, D)))

    def apply_expert(operands):
        rows_in, w_gate, w_up, w_down = operands
        gate_part = jnp.dot(rows_in, w_gate, preferred_element_type=jnp.float32)
        up_part = jnp.dot(rows_in, w_up, preferred_element_type=jnp.float32)
        hidden = (jax.nn.silu(gate_part) * up_part).astype(jnp.bfloat16)
        return jnp.dot(hidden, w_down, preferred_element_type=jnp.float32).astype(jnp.bfloat16)
    results = lax.map(apply_expert, (buffer, expert_gate, expert_up, expert_down))
    first_pick = results[routes[:, 0], row_slot[:, 0]].astype(jnp.float32)
    second_pick = results[routes[:, 1], row_slot[:, 1]].astype(jnp.float32)
    routed = route_weight[:, 0:1] * first_pick + route_weight[:, 1:2] * second_pick
    return (stream + routed).astype(jnp.bfloat16)
```

```python
import jax
import jax.numpy as jnp
import numpy as np
from jax import lax
from jax.experimental import pallas as pl
from jax.experimental.pallas import tpu as pltpu
from jax.sharding import PartitionSpec as P

MESH = pl.DeviceIdType.MESH
BF = jnp.bfloat16
F32 = jnp.float32
EPS = 1e-06
THETA = 10000.0
D = 4096
NS, NT, NZ = 32, 16, 16
TOK = 128
NCH = 4
ROWS = NS * 16 // NCH
ORDER = [0, 1, -1, 2, 8, 7, -7, 6, -6, 5, -5, 4, -4, 3, -3, -2]
FAR_FIRST = [8, 7, -7, 6, -6, 5, -5, 4, -4, 3, -3, 2, -2, 1, -1, 0]


def dot(a, b, dims=((1,), (0,)), precision=None):
    return lax.dot_general(a, b, (dims, ((), ())), precision=precision, preferred_element_type=F32)


def silu(v):
    return v / (1.0 + jnp.exp(-v))


def tables():
    i = np.arange(TOK, dtype=np.float64)[:, None]
    s = np.arange(NS, dtype=np.float64)[:, None] * TOK
    small = THETA ** (-np.arange(64, dtype=np.float64) * 2.0 / 128)
    small = np.concatenate([small, small])[None]
    large = THETA ** (-np.arange(128, dtype=np.float64) * 2.0 / 256)[None]

    def four(p):
        return np.concatenate(
            [np.cos(p * small), np.sin(p * small), np.cos(p * large), np.sin(p * large)], axis=1
        ).astype(np.float32)

    return four(i), four(s)[:, None, :]


def kernel(
    res, qs, ks, ql, kl, vals, gates, ld, hgain, wo_in, ngain, routes, rw, wg, wu, wd, tab_i, tab_s,
    out,
    u_send, u_recv, e_send, e_recv, wo, ho, ss_send, ss_recv, stream, choose, xs, x4, wgu, wd2,
    psend, precv, hid, p2send, p2recv, rsend, ret, qa, qb, within,
    ring_sem, part_sem, u_sem, e_sem, c_sem, ss_sem, x_sem, g_sem, m_sem, a_sem, d_sem, r_sem,
    w_sem, loc_sem, snd,
):
    me_s = lax.axis_index("sp")
    me_t = lax.axis_index("tp")
    z, c = lax.div(me_s, 2), lax.rem(me_s, 2)
    y, x = lax.div(me_t, 4), lax.rem(me_t, 4)

    def at_z(dz, j):
        return lax.rem(z + (dz + NZ), NZ) * 2 + lax.rem(c + j, 2)

    def t_of(yy, xx):
        return yy * 4 + xx

    def y_peer(i):
        return lax.rem(y + i, 4)

    def x_peer(i):
        return lax.rem(x + i, 4)

    def send(src, dst, s_sem, r_sem_, s, t):
        pltpu.make_async_remote_copy(
            src_ref=src, dst_ref=dst, send_sem=s_sem, recv_sem=r_sem_, device_id=(s, t), device_id_type=MESH
        ).start()

    def wait(ref, sem):
        pltpu.make_async_copy(ref, ref, sem).wait()

    def lanes(index, size):
        return pl.ds(pl.multiple_of(index * size, size), size)

    barrier = pltpu.get_barrier_semaphore()

    def greet_s(i, carry):
        pl.semaphore_signal(barrier, inc=1, device_id=(lax.rem(me_s + i, NS), me_t), device_id_type=MESH)
        return carry

    def greet_t(i, carry):
        pl.semaphore_signal(barrier, inc=1, device_id=(me_s, lax.rem(me_t + i, NT)), device_id_type=MESH)
        return carry

    lax.fori_loop(1, NS, greet_s, 0)
    lax.fori_loop(1, NT, greet_t, 0)

    local = [
        pltpu.make_async_copy(wg.at[lanes(y, 1024), :], wgu.at[:, lanes(2 * y, 128)], loc_sem.at[0]),
        pltpu.make_async_copy(wu.at[lanes(y, 1024), :], wgu.at[:, lanes(2 * y + 1, 128)], loc_sem.at[1]),
        pltpu.make_async_copy(wd.at[:, x], wd2.at[:, :, lanes(x, 256)], loc_sem.at[2]),
    ]
    for copy in local:
        copy.start()

    row = lax.broadcasted_iota(jnp.int32, (TOK, TOK), 0)
    col = lax.broadcasted_iota(jnp.int32, (TOK, TOK), 1)
    causal = row >= col
    tri = causal.astype(F32)

    def cumul_of(g):
        rates = jnp.broadcast_to(ld[:, g : g + 1], (TOK, TOK))
        return dot(tri, rates, precision=lax.Precision.HIGHEST)

    cum = [cumul_of(0), cumul_of(1)]

    base = tab_s[me_s]

    def turned(k):
        ci, si = tab_i[:, k * 256 : k * 256 + 128], tab_i[:, k * 256 + 128 : k * 256 + 256]
        cs, sn = base[:, k * 256 : k * 256 + 128], base[:, k * 256 + 128 : k * 256 + 256]
        return ci * cs - si * sn, si * cs + ci * sn

    cos_a, sin_a = turned(0)
    cos_b, sin_b = turned(1)
    sin_a = jnp.where(col < 64, -sin_a, sin_a)

    def rot_a(v):
        v = v.astype(F32)
        return v * cos_a + pltpu.roll(v, 64, 1) * sin_a

    def rot_b(v):
        lo, hi = v[:, :128].astype(F32), v[:, 128:].astype(F32)
        return jnp.concatenate([lo * cos_b - hi * sin_b, hi * cos_b + lo * sin_b], axis=1)

    key_a = (rot_a(ks[...]) * (128.0 ** -0.5)).astype(BF)
    key_b = (rot_b(kl[...]) * (256.0 ** -0.5)).astype(BF)
    query_a = rot_a(qs[...]).astype(BF)
    query_b = rot_b(ql[...]).astype(BF)
    value = [vals[:, :128], vals[:, 128:]]

    def spread_to(rows_, width, first):
        d = lax.broadcasted_iota(jnp.int32, (rows_, 512), 0)
        place = lax.broadcasted_iota(jnp.int32, (rows_, 512), 1)
        inner = lax.rem(place, 16) - first
        hit = (inner >= 0) & (inner < width) & (d == lax.div(place, 16) * width + inner)
        return jnp.where(hit, 1.0, 0.0).astype(BF)

    perm_a = spread_to(128, 4, 8)
    perm_b = spread_to(256, 8, 0)

    fall_a = jnp.exp(cum[0][TOK - 1 :, :] - cum[0])
    fall_b = jnp.exp(cum[1][TOK - 1 :, :] - cum[1])
    carried_a = (key_a.astype(F32) * fall_a).astype(BF)
    carried_b = (key_b.astype(F32) * jnp.concatenate([fall_b, fall_b], axis=1)).astype(BF)
    update = dot(dot(carried_a, perm_a).astype(BF), value[0], ((0,), (0,))) + dot(
        dot(carried_b, perm_b).astype(BF), value[1], ((0,), (0,))
    )
    place = lax.rem(lax.broadcasted_iota(jnp.int32, (512, TOK), 0), 16)
    for g, at in ((1, 12), (0, 14)):
        last = cum[g][TOK - 1 :, :]
        high = last.astype(BF).astype(F32)
        update = jnp.where(place == at, high, update)
        update = jnp.where(place == at + 1, last - high, update)
    u_send[...] = update.astype(BF).reshape(NS, 16, TOK)

    pl.semaphore_wait(barrier, NS - 1 + NT - 1)

    def scatter(src, dst, sems):
        for dz in FAR_FIRST:
            for j in (0, 1):
                if dz == 0 and j == 0:
                    continue
                to = at_z(dz, j)
                send(src.at[to], dst.at[me_s], sems.at[0], sems.at[1], to, me_t)
        dst[pl.ds(me_s, 1)] = src[pl.ds(me_s, 1)]

    scatter(u_send, u_recv, u_sem)

    partner = z * 2 + (1 - c)

    def block_of(zz, cc, g):
        head = zz if g == 0 else lax.rem(zz, 4) * 4 + lax.div(zz, 4)
        return wo.at[g, pl.ds(pl.multiple_of(head * 128 + cc * 64, 64), 64), :]

    def ring_send(k):
        for g in (0, 1):
            for way, dz in ((0, 1), (1, -1)):
                if k > 1 and way == 1 and k - 1 > 7:
                    continue
                owner = lax.rem(z - dz * (k - 1) + NZ, NZ)
                block = block_of(owner, c, g)
                src = wo_in.at[g] if k == 1 else block
                if (way == 0 and k <= 8) or (way == 1 and k <= 7):
                    send(src, block, snd.at[0], ring_sem.at[way, k - 1, g], at_z(dz, 0), me_t)
                if k > 1 or way == 0:
                    send(src, block, snd.at[0], part_sem.at[0], partner, me_t)

    def ring_recv(k):
        for g in (0, 1):
            wait(wo_in.at[g], ring_sem.at[0, k - 1, g])
            if k <= 7:
                wait(wo_in.at[g], ring_sem.at[1, k - 1, g])

    def ring_step(k):
        ring_recv(k)
        ring_send(k + 1)

    own = [pltpu.make_async_copy(wo_in.at[g], block_of(z, c, g), loc_sem.at[3 + g]) for g in (0, 1)]
    for copy in own:
        copy.start()
    ring_send(1)

    def spread_weight(src, half):
        for i in (2, 1, 3):
            to = y_peer(i)
            send(src.at[lanes(to, 1024), :], wgu.at[:, lanes(2 * y + half, 128)], w_sem.at[half],
                 w_sem.at[2 + half], me_s, t_of(to, x))

    for i in (2, 1, 3):
        to = x_peer(i)
        send(wd.at[:, to], wd2.at[:, :, lanes(x, 256)], w_sem.at[4], w_sem.at[5], me_s, t_of(y, to))
    spread_weight(wg, 0)

    qa[...] = dot(query_a, perm_a).astype(BF)
    qb[...] = dot(query_b, perm_b).astype(BF)
    for g, (q, k) in enumerate(((query_a, key_a), (query_b, key_b))):
        apart = jnp.where(causal, cum[g] - cum[g].T, 0.0)
        weight = jnp.where(causal, jnp.exp(apart), 0.0)
        weighted = (dot(q, k, ((1,), (1,))) * weight).astype(BF)
        within[g] = dot(weighted, value[g])

    experts = lax.broadcasted_iota(jnp.int32, (TOK, TOK), 1)
    hot = [(routes[:, n : n + 1] == experts).astype(F32) for n in (0, 1)]
    strict = (row > col).astype(BF)
    before = dot(strict, (hot[0] + hot[1]).astype(BF))
    slots = lax.broadcasted_iota(jnp.int32, (TOK, 512), 1)
    for n in (0, 1):
        slot = jnp.sum(before * hot[n], axis=1, keepdims=True).astype(jnp.int32)
        target = routes[:, n : n + 1] * 16 + slot
        choose[n] = jnp.where(slots == target, 1.0, 0.0).astype(BF)

    for k in (1, 2):
        ring_step(k)

    wait(u_recv.at[0 : NS - 1], u_sem.at[1])
    state = jnp.zeros((16, TOK), F32)
    first_rows = lax.broadcasted_iota(jnp.int32, (16, TOK), 0) < 8
    for s in range(NS):
        e_send[s] = state.astype(BF)
        if s < NS - 1:
            piece = u_recv[s].astype(F32)
            drop_b = jnp.exp(piece[12:13] + piece[13:14])
            drop_a = jnp.exp(piece[14:15] + piece[15:16])
            state = jnp.where(first_rows, drop_b, drop_a) * state + piece
    scatter(e_send, e_recv, e_sem)

    for k in (3, 4, 5):
        ring_step(k)

    wait(e_recv.at[0 : NS - 1], e_sem.at[1])
    entering = e_recv[...].reshape(512, TOK)
    spots = (me_t, x * 4 + y)
    for g, q in ((0, qa), (1, qb)):
        retained = within[g] + jnp.exp(cum[g]) * dot(q[...], entering)
        scaled = retained * lax.rsqrt(jnp.mean(retained * retained, axis=1, keepdims=True) + EPS)
        gate = gates[:, g * 128 : (g + 1) * 128].astype(F32)
        ho[g, :, lanes(spots[g], 128)] = (scaled * hgain[g : g + 1, :] * silu(gate)).astype(BF)

    for i in (2, 1, 3):
        mine = ho.at[0, :, lanes(spots[0], 128)]
        send(mine, mine, snd.at[1], c_sem.at[0], me_s, t_of(y, x_peer(i)))
        mine = ho.at[1, :, lanes(spots[1], 128)]
        send(mine, mine, snd.at[1], c_sem.at[1], me_s, t_of(y_peer(i), x))
    ring_step(6)
    wait(ho.at[0, :, 0:384], c_sem.at[0])
    for i in (2, 1, 3):
        mine = ho.at[0, :, lanes(y, 512)]
        send(mine, mine, snd.at[2], c_sem.at[2], me_s, t_of(y_peer(i), x))
    wait(ho.at[1, :, 0:384], c_sem.at[1])
    for i in (2, 1, 3):
        mine = ho.at[1, :, lanes(x, 512)]
        send(mine, mine, snd.at[2], c_sem.at[3], me_s, t_of(y, x_peer(i)))
    ring_step(7)
    ring_recv(8)
    for g in (0, 1):
        block = block_of(lax.rem(z + 8, NZ), c, g)
        send(block, block, snd.at[0], part_sem.at[0], partner, me_t)
    for copy in own:
        copy.wait()
    wait(wo.at[0], part_sem.at[0])
    wait(ho.at[0, :, 0:1536], c_sem.at[2])
    mixed = dot(ho[0], wo[0])
    wait(ho.at[1, :, 0:1536], c_sem.at[3])
    mixed = mixed + dot(ho[1], wo[1])
    now = res[...].astype(F32) + mixed.astype(BF).astype(F32)
    stream[...] = now
    squares = jnp.sum(now * now, axis=1, keepdims=True)
    line = jnp.broadcast_to(squares, (TOK, TOK)).T[0:1, :]
    ss_send[...] = line
    ss_recv[me_t] = line
    for i in (10, 9, 11, 5, 6, 7, 13, 14, 15, 2, 8, 1, 3, 4, 12):
        send(ss_send, ss_recv.at[me_t], snd.at[3], ss_sem.at[0], me_s, lax.rem(me_t + i, NT))
    spread_weight(wu, 1)
    wait(ss_recv.at[0 : NT - 1], ss_sem.at[0])
    total = jnp.sum(ss_recv[...], axis=0)
    total = jnp.broadcast_to(total, (TOK, TOK)).T[:, 0:1]
    normed = (now * lax.rsqrt(total / D + EPS) * ngain[...]).astype(BF)
    xs[...] = dot(choose[0] + choose[1], normed, ((0,), (0,))).astype(BF).reshape(NS, 16, 256)

    here = lanes(x, 256)

    def block_rows(idx, cc):
        return pl.ds(pl.multiple_of((2 * idx + cc) * 16, 16), 16)

    keep = pltpu.make_async_copy(xs.at[me_s], x4.at[block_rows(0, c), here], loc_sem.at[5])
    keep.start()
    for idx, off in enumerate(ORDER):
        for j in (0, 1):
            if off == 0 and j == 0:
                continue
            to = at_z(-off, j)
            send(xs.at[to], x4.at[block_rows(idx, c), here], snd.at[4], x_sem.at[idx // 4], to, me_t)

    def chunk(k):
        return pl.ds(k * ROWS, ROWS)

    def stage_g(k):
        if k == 0:
            keep.wait()
            wait(x4.at[0:112, 0:256], x_sem.at[0])
        else:
            wait(x4.at[0:128, 0:256], x_sem.at[k])
        for i in (2, 1, 3):
            block = x4.at[chunk(k), here]
            send(block, block, snd.at[5], g_sem.at[k], me_s, t_of(y, x_peer(i)))

    def stage_m(k):
        wait(x4.at[chunk(k), 0:768], g_sem.at[k])
        if k == 0:
            local[0].wait()
            local[1].wait()
            for half in (0, 1):
                wait(wgu.at[:, 0:384], w_sem.at[2 + half])
        psend[chunk(k), :] = dot(x4[chunk(k), :], wgu[...]).astype(BF)
        for i in (2, 1, 3):
            to = y_peer(i)
            send(psend.at[chunk(k), lanes(to, 256)], precv.at[i - 1, chunk(k), :], snd.at[6], m_sem.at[k],
                 me_s, t_of(to, x))

    def stage_a(k):
        wait(precv.at[:, chunk(k), :], m_sem.at[k])
        both = psend[chunk(k), lanes(y, 256)].astype(F32)
        for i in range(3):
            both = both + precv[i, chunk(k), :].astype(F32)
        hid[chunk(k), lanes(y, 128)] = (silu(both[:, :128]) * both[:, 128:]).astype(BF)
        for i in (2, 1, 3):
            block = hid.at[chunk(k), lanes(y, 128)]
            send(block, block, snd.at[7], a_sem.at[k], me_s, t_of(y_peer(i), x))

    def stage_d(k):
        wait(hid.at[chunk(k), 0:384], a_sem.at[k])
        if k == 0:
            local[2].wait()
            wait(wd2.at[:, :, 0:768], w_sem.at[5])
        p2send[chunk(k), :] = dot(hid[chunk(k), :], wd2[...].reshape(512, 1024)).astype(BF)
        for i in (2, 1, 3):
            to = x_peer(i)
            send(p2send.at[chunk(k), lanes(to, 256)], p2recv.at[i - 1, chunk(k), :], snd.at[8], d_sem.at[k],
                 me_s, t_of(y, to))

    stay = pltpu.make_async_copy(rsend.at[block_rows(0, c)], ret.at[lanes(me_s, 16)], loc_sem.at[6])

    def stage_r(k):
        wait(p2recv.at[:, chunk(k), :], d_sem.at[k])
        done = p2send[chunk(k), lanes(x, 256)].astype(F32)
        for i in range(3):
            done = done + p2recv[i, chunk(k), :].astype(F32)
        rsend[chunk(k), :] = done.astype(BF)
        if k == 0:
            stay.start()
        for idx in range(4 * k, 4 * k + 4):
            for j in (0, 1):
                if idx == 0 and j == 0:
                    continue
                block = block_rows(idx, lax.rem(c + j, 2))
                send(rsend.at[block], ret.at[lanes(me_s, 16)], snd.at[9], r_sem.at[0], at_z(ORDER[idx], j), me_t)

    stages = (stage_g, stage_m, stage_a, stage_d, stage_r)
    for tick in range(NCH + len(stages) - 1):
        for n in reversed(range(len(stages))):
            if 0 <= tick - n < NCH:
                stages[n](tick - n)

    stay.wait()
    wait(ret.at[0:496], r_sem.at[0])
    back = ret[...]
    routed = rw[:, 0:1] * dot(choose[0], back) + rw[:, 1:2] * dot(choose[1], back)
    out[...] = (stream[...] + routed).astype(BF)

    wait(u_send.at[0 : NS - 1], u_sem.at[0])
    wait(e_send.at[0 : NS - 1], e_sem.at[0])
    wait(wo.at[:, 0:1984], snd.at[0])
    wait(ho.at[0, :, 0:768], snd.at[1])
    wait(ho.at[:, :, 0:1536], snd.at[2])
    wait(ss_recv.at[0 : NT - 1], snd.at[3])
    wait(xs.at[0 : NS - 1], snd.at[4])
    wait(x4.at[:, 0:768], snd.at[5])
    wait(psend.at[:, 0:768], snd.at[6])
    wait(hid.at[:, 0:384], snd.at[7])
    wait(p2send.at[:, 0:768], snd.at[8])
    wait(ret.at[0:496], snd.at[9])
    for half in (0, 1):
        wait(wgu.at[:, 0:384], w_sem.at[half])
    wait(wd2.at[:, :, 0:768], w_sem.at[4])


def per_device(
    residual, query_small, key_narrow_group, query_large, key_large, values, gates, log_decay,
    head_gain, out_weight, norm_gain, routes, route_weight, expert_gate, expert_up, expert_down,
):
    tab_i, tab_s = tables()
    vmem = pl.BlockSpec(memory_space=pltpu.VMEM)
    far = pl.BlockSpec(memory_space=pl.ANY)
    v = pltpu.VMEM
    dma = pltpu.SemaphoreType.DMA
    return pl.pallas_call(
        kernel,
        out_shape=jax.ShapeDtypeStruct((TOK, 256), BF),
        in_specs=[vmem] * 13 + [far] * 3 + [vmem] * 2,
        out_specs=vmem,
        scratch_shapes=[
            v((NS, 16, TOK), BF), v((NS, 16, TOK), BF), v((NS, 16, TOK), BF), v((NS, 16, TOK), BF),
            v((2, 2048, 256), BF), v((2, TOK, 2048), BF),
            v((1, TOK), F32), v((NT, 1, TOK), F32),
            v((TOK, 256), F32), v((2, TOK, 512), BF),
            v((NS, 16, 256), BF), v((512, 1024), BF), v((1024, 1024), BF), v((4, 128, 1024), BF),
            v((512, 1024), BF), v((3, 512, 256), BF), v((512, 512), BF),
            v((512, 1024), BF), v((3, 512, 256), BF), v((512, 256), BF), v((512, 256), BF),
            v((TOK, 512), BF), v((TOK, 512), BF), v((2, TOK, TOK), F32),
            dma((2, 8, 2)), dma((1,)), dma((2,)), dma((2,)), dma((4,)), dma((1,)), dma((NCH,)),
            dma((NCH,)), dma((NCH,)), dma((NCH,)), dma((NCH,)), dma((1,)),
            dma((6,)), dma((7,)), dma((10,)),
        ],
        compiler_params=pltpu.CompilerParams(collective_id=0, has_side_effects=True),
        name="layer",
    )(
        residual, query_small, key_narrow_group, query_large, key_large,
        values.reshape(TOK, 256), gates.reshape(TOK, 256), log_decay.reshape(TOK, 2),
        head_gain, out_weight, norm_gain.reshape(1, 256), routes, route_weight,
        expert_gate.reshape(4096, 128), expert_up.reshape(4096, 128),
        expert_down.reshape(4, 4, 128, 256), jnp.asarray(tab_i), jnp.asarray(tab_s),
    )


def solution(mesh):
    sp, tp = "sp", "tp"
    placed = (
        P(sp, tp), P(sp, tp), P(sp, tp), P(sp, tp), P(sp, tp),
        P(sp, None, tp), P(sp, None, tp), P(sp, None, tp),
        P(None, tp), P(None, sp, tp), P(tp), P(sp, None), P(sp, None),
        P(sp, None, tp), P(sp, None, tp), P(sp, None, tp),
    )
    return jax.shard_map(per_device, mesh=mesh, in_specs=placed, out_specs=P(sp, tp), check_vma=False)
```
